32 devices in a mesh: ep: 8 (over z, core), tp: 4 (over y, x).
Axes of the slice: x: 2, y: 2, z: 4, core: 2. Of those that a mesh axis runs over, the one named last changes fastest.
Arguments:
- mix_in: bfloat16 [2048, 2048], P('ep'), may hold values from -6 to 6
- mix_gain: float32 [2048], replicated, may hold values from 0.1 to 1.9
- w_in_x: bfloat16 [2048, 2048], P(None, 'tp'), may hold values from -0.125 to 0.125
- w_in_y: bfloat16 [2048, 2048], P(None, 'tp'), may hold values from -0.125 to 0.125
- conv_taps: float32 [4, 2048], P(None, 'tp'), may hold values from -3 to 3
- recur_gate_w: bfloat16 [16, 128, 128], P('tp'), may hold values from -0.5 to 0.5
- input_gate_w: bfloat16 [16, 128, 128], P('tp'), may hold values from -0.5 to 0.5
- decay_logit: float32 [2048], P('tp'), may hold values from 4 to 20
- decay_shift: float32 [2048, 2048], P('ep', 'tp'), may hold values from -2.2 to 0
- moe_in: bfloat16 [2048, 2048], P('ep'), may hold values from -6 to 6
- moe_gain: float32 [2048], replicated, may hold values from 0.1 to 1.9
- routes: int32 [2048, 2], P('ep'), may hold values from 0 to 7, all different within a row; in each aligned block of 256 rows (0 to 255, 256 to 511, ...) at most 128 rows name the same one
- route_weight: float32 [2048, 2], P('ep'), may hold values from 0.1 to 1
- expert_gate: bfloat16 [8, 2048, 2048], P('ep', None, 'tp'), may hold values from -0.125 to 0.125
- expert_up: bfloat16 [8, 2048, 2048], P('ep', None, 'tp'), may hold values from -0.125 to 0.125
- expert_down: bfloat16 [8, 2048, 2048], P('ep', None, 'tp'), may hold values from -0.125 to 0.125
Outputs:
- mixer_out: bfloat16 [2048, 2048], P('ep', 'tp')
- moe_out: bfloat16 [2048, 2048], P('ep', 'tp')
The draws below stay inside these ranges and needn't reach their ends.
Inputs may be any that keep to these rules, and one draw needn't show every extreme that they name: `routes`: each row names 2 different experts. Among the rows of one index of ep no expert is named more than 128 times, a bound that some block reaches.
All inputs are finite; a program needn't handle non-finite values.
Results may differ from the reference program's by a relative error of at most 0.0095.
Values may be sent and summed in bfloat16 or wider, within the bound.
No kernel may reach another device: no remote copies, remote signals or barrier semaphores. Data moves between devices by JAX's collectives and lax.ppermute only.
A program may use at most 64 MiB of HBM per device.

```python
import math
import jax
import jax.numpy as jnp
import numpy as np
from jax import lax

D = 2048
FILTER_SECTIONS = 16
SECTION_FEATURES = 128
KCONV = 4
FF = 2048
TOPK = 2
TOK_DEV = 256
SUBBATCH_SPAN = 2048
WIDTH = 2048
EXPERTS = 8
CAP = 128
N_EP = 8


def draw_decay_logit(key, part):
    pick_key, slow_key, fast_key, jitter_key = jax.random.split(jax.random.fold_in(key, 11), 4)
    fast_head = jax.random.uniform(pick_key, (FILTER_SECTIONS,)) < 0.5
    slow_rate = jnp.exp(jax.random.uniform(slow_key, (FILTER_SECTIONS,), minval=math.log(0.2), maxval=math.log(0.6))) / SUBBATCH_SPAN
    fast_rate = jnp.exp(jax.random.uniform(fast_key, (FILTER_SECTIONS,), minval=math.log(0.01), maxval=math.log(1.0 / 30.0)))
    head_rate = jnp.where(fast_head, fast_rate, slow_rate)
    jitter = jax.random.uniform(jitter_key, (FILTER_SECTIONS, SECTION_FEATURES), minval=0.7, maxval=1.4)
    softened = (head_rate[:, None] * jitter / 4.0).reshape(FILTER_SECTIONS * SECTION_FEATURES)
    return -jnp.log(jnp.expm1(softened))


def draw_decay_shift(key, part):
    block_key, chan_key, place_key, depth_key = jax.random.split(jax.random.fold_in(key, 23), 4)
    blocks = SUBBATCH_SPAN // TOK_DEV
    spread = math.log(2.0)
    factor = jnp.exp(jax.random.uniform(block_key, (blocks,), minval=-spread, maxval=spread))
    channel = jax.random.uniform(chan_key, (FILTER_SECTIONS * SECTION_FEATURES,), minval=0.2, maxval=0.8)
    stationary_regime = -jnp.repeat(factor, TOK_DEV)[:, None] * channel[None, :] / SUBBATCH_SPAN
    assignment_seats = jax.random.randint(place_key, (3, FILTER_SECTIONS), 0, SUBBATCH_SPAN)
    stack_levels = jnp.log1p(-jax.random.uniform(depth_key, (3, FILTER_SECTIONS), minval=0.2, maxval=0.5))
    sequence_offsets = jnp.arange(SUBBATCH_SPAN)[:, None]
    packet_clusters = jnp.zeros((SUBBATCH_SPAN, FILTER_SECTIONS), jnp.float32)
    for picked_ordinal in range(3):
        packet_clusters = packet_clusters + jnp.where(sequence_offsets == assignment_seats[picked_ordinal][None, :], stack_levels[picked_ordinal][None, :], 0.0)
    return stationary_regime + jnp.repeat(packet_clusters, SECTION_FEATURES, axis=1)


def shard_levels(rng, shape, shards, least, high):
    factor_of = 1.0
    for axis_at, parts in shards:
        heights = jax.random.uniform(jax.random.fold_in(jax.random.fold_in(rng, 6), axis_at), (parts,), jnp.float32, least / len(shards), high / len(shards))
        factor_of = factor_of * jnp.repeat(jnp.exp(heights), shape[axis_at] // parts).reshape((-1,) + (1,) * (len(shape) - 1 - axis_at))
    return factor_of


def assign_block(rng, own, number, rows, amount, top, most, skew):
    sequence = jax.random.permutation(rng, amount)
    crowded, common = load_shares(amount, rows * top, most, skew, True), load_shares(amount, rows * top, most, skew, False)
    places = jnp.arange(amount)

    def named(sizes, offset_by):
        used = int((sizes > 0).sum())
        fixed = max(1, used // 4)
        passed = fixed + (places - fixed + offset_by * (used - fixed)) % max(1, amount - fixed)
        return jnp.zeros((amount,), jnp.int32).at[sequence[jnp.where(places < fixed, places, passed)]].set(jnp.asarray(sizes, jnp.int32))

    sizes = jnp.where(number % 4 == 0, named(crowded, number // 4), named(common, number - number // 4 - 1))
    mixed = jax.random.permutation(jax.random.fold_in(own, 3), amount)
    giver, taker = mixed[0:amount // 2 * 2:2], mixed[1:amount // 2 * 2:2]
    slack = jnp.minimum(sizes[giver] - 1, most - sizes[taker]) // 2
    slack = jnp.where((giver == sequence[0]) | (taker == sequence[0]) | (sizes[taker] == 0), 0, jnp.maximum(slack, 0))
    passed = jax.random.randint(jax.random.fold_in(own, 4), (amount // 2,), 0, 1 << 20) % (slack + 1)
    sizes = sizes.at[giver].add(-passed).at[taker].add(passed)
    labels = jnp.searchsorted(jnp.cumsum(sizes), jnp.arange(rows * top), side="right").astype(jnp.int32)
    listing = labels.reshape(top, rows).T
    listing = listing[jax.random.permutation(jax.random.fold_in(own, 1), rows)]
    offset_by = jax.random.randint(jax.random.fold_in(own, 2), (rows, 1), 0, top)
    return jnp.take_along_axis(listing, (jnp.arange(top)[None, :] + offset_by) % top, axis=1)


def load_shares(number_of, total, most, slope, full):
    portions = [(1 << 20) // math.isqrt(grade ** slope) + 1 for grade in range(1, number_of + 1)]
    largest = most if full else min(most, max(-(-total // number_of), total * portions[0] // sum(portions)))
    least = 1 if total - largest >= number_of - 1 else 0
    holding, spare = [largest] + [least] * (number_of - 1), total - largest - least * (number_of - 1)
    while spare > 0:
        free = [i for i in range(1, number_of) if holding[i] < largest] or [i for i in range(1, number_of) if holding[i] < most]
        mass, remaining = sum([portions[i] for i in free]), spare
        for i in free:
            more = min(most - holding[i], max(1, remaining * portions[i] // mass), spare)
            holding[i] = holding[i] + more
            spare = spare - more
    return np.array(holding)


def noise(rng, shape, scale, bound, shards=(), held_as=jnp.bfloat16):
    level = shard_levels(rng, shape, shards, -0.22, 0.18) if shards else 1.0
    drawn = jax.random.normal(rng, shape, jnp.float32) * scale * level
    return jnp.minimum(jnp.maximum(drawn, -bound), bound).astype(held_as)


def setup_inputs(seed: int = 0) -> dict:
    keys = jax.random.split(jax.random.key(seed), 17)
    mix_in = noise(keys[0], (SUBBATCH_SPAN, D), 1.0, 6.0, ((0, 8),))
    mix_gain = jnp.clip(1.0 + 0.18 * jax.random.normal(keys[1], (D,), jnp.float32), 0.1, 1.9)
    w_in_x = noise(keys[2], (D, WIDTH), D ** -0.5, 0.125, ((1, 4),))
    w_in_y = noise(keys[3], (D, WIDTH), D ** -0.5, 0.125, ((1, 4),))
    conv_taps = noise(keys[4], (KCONV, WIDTH), 0.5, 3.0, ((1, 4),), jnp.float32)
    recur_gate_w = noise(keys[5], (FILTER_SECTIONS, SECTION_FEATURES, SECTION_FEATURES), SECTION_FEATURES ** -0.5, 0.5, ((0, 4),))
    input_gate_w = noise(keys[6], (FILTER_SECTIONS, SECTION_FEATURES, SECTION_FEATURES), SECTION_FEATURES ** -0.5, 0.5, ((0, 4),))
    decay_logit = draw_decay_logit(jax.random.fold_in(keys[16], 71), 0)
    decay_shift = draw_decay_shift(jax.random.fold_in(keys[16], 71), 0)
    moe_in = noise(keys[9], (SUBBATCH_SPAN, D), 1.0, 6.0, ((0, 8),))
    moe_gain = jnp.clip(1.0 + 0.18 * jax.random.normal(keys[10], (D,), jnp.float32), 0.1, 1.9)
    routes_keys = jax.random.split(jax.random.fold_in(keys[11], 1), SUBBATCH_SPAN // TOK_DEV)
    routes_turns = jax.random.permutation(jax.random.fold_in(keys[11], 3), SUBBATCH_SPAN // TOK_DEV)
    routes = jax.vmap(lambda own, number: assign_block(jax.random.fold_in(keys[11], 2), own, number, TOK_DEV, EXPERTS, TOPK, CAP, 2))(routes_keys, routes_turns).reshape((SUBBATCH_SPAN, TOPK))
    route_weight = jnp.clip(jnp.exp(math.log(1.0) - 2.3025851 * jax.random.uniform(keys[12], (SUBBATCH_SPAN, TOPK), jnp.float32) ** shard_levels(keys[12], (SUBBATCH_SPAN, TOPK), ((0, 8),), -0.2, 0.2)), 0.1, 1.0)
    expert_gate = noise(keys[13], (EXPERTS, D, FF), D ** -0.5, 0.125, ((0, 8), (2, 4)))
    expert_up = noise(keys[14], (EXPERTS, D, FF), D ** -0.5, 0.125, ((0, 8), (2, 4)))
    expert_down = noise(keys[15], (EXPERTS, FF, D), FF ** -0.5, 0.125, ((0, 8), (2, 4)))
    return {"mix_in": mix_in, "mix_gain": mix_gain, "w_in_x": w_in_x, "w_in_y": w_in_y, "conv_taps": conv_taps, "recur_gate_w": recur_gate_w, "input_gate_w": input_gate_w, "decay_logit": decay_logit, "decay_shift": decay_shift, "moe_in": moe_in, "moe_gain": moe_gain, "routes": routes, "route_weight": route_weight, "expert_gate": expert_gate, "expert_up": expert_up, "expert_down": expert_down}


epsilon = 1e-06
lru_scale = 8.0

def norm_rows(rows, gain):
    widened = rows.astype(jnp.float32)
    scaled = widened * lax.rsqrt(lax.optimization_barrier(jnp.mean(widened * widened, axis=-1, keepdims=True)) + epsilon)
    return (scaled * gain.astype(jnp.float32)[None, :]).astype(jnp.bfloat16)

def link(earlier, later):
    return (earlier[0] * later[0], later[0] * earlier[1] + later[1])

def reference(mix_in, mix_gain, w_in_x, w_in_y, conv_taps, recur_gate_w, input_gate_w, decay_logit, decay_shift, moe_in, moe_gain, routes, route_weight, expert_gate, expert_up, expert_down):
    mixer_rows = norm_rows(mix_in, mix_gain)
    x_branch = jnp.dot(mixer_rows, w_in_x, preferred_element_type=jnp.float32).astype(jnp.bfloat16)
    y_branch = jnp.dot(mixer_rows, w_in_y, preferred_element_type=jnp.float32).astype(jnp.bfloat16)
    padded = jnp.concatenate([jnp.zeros((KCONV - 1, WIDTH), jnp.bfloat16), x_branch], axis=0)
    conv_sum = jnp.zeros((SUBBATCH_SPAN, WIDTH), jnp.float32)
    for tap_index in range(KCONV):
        conv_sum = conv_sum + conv_taps[tap_index][None, :].astype(jnp.float32) * padded[tap_index:tap_index + SUBBATCH_SPAN].astype(jnp.float32)
    x_conv = conv_sum.astype(jnp.bfloat16)
    heads_in = x_conv.astype(jnp.float32).reshape(SUBBATCH_SPAN, FILTER_SECTIONS, SECTION_FEATURES)
    gate_a = jnp.einsum('thi,hij->thj', heads_in, recur_gate_w.astype(jnp.float32)).reshape(SUBBATCH_SPAN, WIDTH)
    gate_x = jnp.einsum('thi,hij->thj', heads_in, input_gate_w.astype(jnp.float32)).reshape(SUBBATCH_SPAN, WIDTH)
    log_decay = -lru_scale * jax.nn.sigmoid(gate_a) * jax.nn.softplus(-decay_logit)[None, :] + decay_shift
    lru_drive = jnp.sqrt(-jnp.expm1(2.0 * log_decay)) * jax.nn.sigmoid(gate_x) * x_conv.astype(jnp.float32)
    through, lru_state = lax.associative_scan(link, (jnp.exp(log_decay), lru_drive), axis=0)
    mixer_out = (lru_state * jax.nn.gelu(y_branch.astype(jnp.float32))).astype(jnp.bfloat16)
    moe_rows = norm_rows(moe_in, moe_gain)
    grouped = routes.reshape(N_EP, TOK_DEV * TOPK)
    onehot = (grouped[:, :, None] == jnp.arange(EXPERTS, dtype=jnp.int32)[None, None, :]).astype(jnp.int32)
    slot_rank = lax.optimization_barrier(jnp.sum(jnp.cumsum(onehot, axis=1) * onehot, axis=2)) - 1
    source = jnp.broadcast_to(jnp.arange(N_EP, dtype=jnp.int32)[:, None], slot_rank.shape)
    slot_index = (source * CAP + slot_rank).reshape(-1).astype(jnp.int32)
    expert_ids = routes.reshape(-1).astype(jnp.int32)
    token_index = jnp.repeat(jnp.arange(SUBBATCH_SPAN, dtype=jnp.int32), TOPK)
    table = jnp.zeros((EXPERTS, N_EP * CAP, D), jnp.bfloat16).at[expert_ids, slot_index].set(moe_rows[token_index])

    def run_expert(packed):
        rows_in, gate_w, up_w, down_w = packed
        gate_proj = jnp.dot(rows_in, gate_w, preferred_element_type=jnp.float32)
        up_proj = jnp.dot(rows_in, up_w, preferred_element_type=jnp.float32)
        hidden = (jax.nn.silu(gate_proj) * up_proj).astype(jnp.bfloat16)
        return jnp.dot(hidden, down_w, preferred_element_type=jnp.float32).astype(jnp.bfloat16)
    results = lax.map(run_expert, (table, expert_gate, expert_up, expert_down))
    picked = results[expert_ids, slot_index].astype(jnp.float32).reshape(SUBBATCH_SPAN, TOPK, D)
    route_share = route_weight / lax.optimization_barrier(jnp.sum(route_weight, axis=1, keepdims=True))
    moe_out = lax.optimization_barrier(jnp.sum(route_share[:, :, None] * picked, axis=1)).astype(jnp.bfloat16)
    return (mixer_out, moe_out)
```

```python
import jax
import jax.numpy as jnp
from jax import lax
from jax.experimental import pallas as pl
from jax.experimental.pallas import tpu as pltpu
from jax.sharding import PartitionSpec as P

epsilon = 1e-06
lru_scale = 8.0
chunks = 2
bf16, f32 = jnp.bfloat16, jnp.float32


def norm_rows(rows, gain):
    widened = rows.astype(f32)
    scaled = widened * lax.rsqrt(jnp.mean(widened * widened, axis=-1, keepdims=True) + epsilon)
    return (scaled * gain[None, :]).astype(bf16)


def from_behind(value, axis, by):
    count = lax.axis_size(axis)
    pairs = [(i, i + by) for i in range(count) if i + by < count]
    return lax.ppermute(value, axis, pairs)


def rotate(value, axis, by):
    count = lax.axis_size(axis)
    return lax.ppermute(value, axis, [(i, (i + by) % count) for i in range(count)])


def swap(value, axis, bit):
    count = lax.axis_size(axis)
    return lax.ppermute(value, axis, [(i, i ^ bit) for i in range(count)])


def spread(blocks, axis, sign):
    count = lax.axis_size(axis)
    out = [None] * count
    out[0] = blocks[0]
    order = sorted(range(1, count), key=lambda k: -min(k, count - k))
    for k in order:
        out[k] = rotate(blocks[k], axis, sign * k)
    return out


def pieces_over(value, axis):
    near, side = swap(value, axis, 1), swap(value, axis, 2)
    half = value.shape[0] // 2
    upper, lower = swap(near[:half], axis, 2), swap(side[half:], axis, 1)
    return [value, near, side, jnp.concatenate([upper, lower], axis=0)]


def dot(a, b):
    return jnp.dot(a, b, preferred_element_type=f32)


def dot_pieces(pieces, weight, index):
    depth = pieces[0].shape[1]
    total = None
    for m, piece in enumerate(pieces):
        part = dot(piece, lax.dynamic_slice_in_dim(weight, (index ^ m) * depth, depth, 0))
        total = part if total is None else total + part
    return total


def scan_kernel(a_ref, b_ref, through_ref, state_ref):
    rows, lanes = a_ref.shape
    a, b = a_ref[...], b_ref[...]
    row = lax.broadcasted_iota(jnp.int32, (rows, lanes), 0)
    step = 1
    while step < rows:
        if step % 8 == 0:
            a_back = jnp.concatenate([jnp.ones((step, lanes), f32), a[: rows - step]], axis=0)
            b_back = jnp.concatenate([jnp.zeros((step, lanes), f32), b[: rows - step]], axis=0)
        else:
            a_back = jnp.where(row >= step, pltpu.roll(a, step, 0), 1.0)
            b_back = jnp.where(row >= step, pltpu.roll(b, step, 0), 0.0)
        b = a * b_back + b
        a = a * a_back
        step *= 2
    through_ref[...] = a
    state_ref[...] = b


def local_scan(a, b):
    rows, width = a.shape
    spec = pl.BlockSpec((rows, 128), lambda i: (0, i))
    shape = jax.ShapeDtypeStruct((rows, width), f32)
    return pl.pallas_call(
        scan_kernel,
        grid=(width // 128,),
        in_specs=[spec, spec],
        out_specs=[spec, spec],
        out_shape=[shape, shape],
        cost_estimate=pl.CostEstimate(
            flops=rows * width * 32, bytes_accessed=rows * width * 16, transcendentals=0
        ),
        name="local_scan",
    )(a, b)


def carried_in(through, state):
    index, count = lax.axis_index("ep"), lax.axis_size("ep")
    pair = jnp.stack([through, state])
    step = 1
    while step < count:
        back = from_behind(pair, "ep", step)
        a, b = pair[0], pair[1]
        joined = jnp.stack([a * back[0], a * back[1] + b])
        pair = jnp.where(index >= step, joined, pair)
        step *= 2
    return from_behind(pair[1:2], "ep", 1)[0]


def mixer(
    mix_in, mix_gain, w_in_x, w_in_y, conv_taps, recur_gate_w, input_gate_w, decay_logit, decay_shift
):
    row_count = mix_in.shape[0]
    width_dev = w_in_x.shape[1]
    heads_dev, block_size = recur_gate_w.shape[:2]
    tap_count = conv_taps.shape[0]
    mixer_rows = norm_rows(mix_in, mix_gain)
    x_branch = dot(mixer_rows, w_in_x).astype(bf16)
    y_branch = dot(mixer_rows, w_in_y).astype(bf16)
    previous = from_behind(x_branch[row_count - (tap_count - 1) :], "ep", 1)
    padded = jnp.concatenate([previous, x_branch], axis=0)
    conv_sum = jnp.zeros((row_count, width_dev), f32)
    for tap_index in range(tap_count):
        conv_sum = conv_sum + conv_taps[tap_index][None, :] * padded[
            tap_index : tap_index + row_count
        ].astype(f32)
    x_conv = conv_sum.astype(bf16)
    gates = []
    for weight in (recur_gate_w, input_gate_w):
        blocks = [
            dot(x_conv[:, h * block_size : (h + 1) * block_size], weight[h])
            for h in range(heads_dev)
        ]
        gates.append(jnp.concatenate(blocks, axis=1))
    gate_a, gate_x = gates
    log_decay = (
        -lru_scale * jax.nn.sigmoid(gate_a) * jax.nn.softplus(-decay_logit)[None, :] + decay_shift
    )
    drive = jnp.sqrt(-jnp.expm1(2.0 * log_decay)) * jax.nn.sigmoid(gate_x) * x_conv.astype(f32)
    through, local_state = local_scan(jnp.exp(log_decay), drive)
    carried = carried_in(through[row_count - 1], local_state[row_count - 1])
    lru_state = local_state + through * carried[None, :]
    return (lru_state * jax.nn.gelu(y_branch.astype(f32))).astype(bf16)


def experts(moe_in, moe_gain, routes, route_weight, expert_gate, expert_up, expert_down):
    ep, tp = lax.axis_size("ep"), lax.axis_size("tp")
    ep_index, tp_index = lax.axis_index("ep"), lax.axis_index("tp")
    moe_rows = norm_rows(moe_in, moe_gain)
    tokens, features = moe_rows.shape
    capacity = 2 * tokens * routes.shape[1] // ep
    width = features // tp
    own = lax.dynamic_slice_in_dim(moe_rows, tp_index * width, width, 1)

    ahead = lax.rem(routes - ep_index + ep, ep)
    steps_ahead = jnp.arange(ep, dtype=jnp.int32)
    chosen = ahead[:, :, None] == steps_ahead[None, None, :]
    named = jnp.any(chosen, axis=1)
    order = jnp.arange(tokens, dtype=jnp.int32)
    before = (order[None, :] < order[:, None]).astype(bf16)
    rank = dot(before, named.astype(bf16)).astype(jnp.int32)
    rank = jnp.where(named, rank, -1)
    share = route_weight / jnp.sum(route_weight, axis=1, keepdims=True)
    weight = jnp.sum(jnp.where(chosen, share[:, :, None], 0.0), axis=1)
    weight_top = lax.reduce_precision(weight, 8, 7)
    weight_low = weight - weight_top
    rank_rows = rank.T

    part = capacity // chunks
    gate_w, up_w, down_w = expert_gate[0], expert_up[0], expert_down[0]
    square = tp == 4
    direct = ep <= 8

    def exchange(rows, sign):
        blocks = rows.reshape(ep, part, rows.shape[1])
        if direct:
            return jnp.concatenate(spread([blocks[k] for k in range(ep)], "ep", sign), axis=0)
        placed = blocks[lax.rem(sign * (steps_ahead - ep_index) + ep, ep)]
        moved = lax.all_to_all(placed, "ep", split_axis=0, concat_axis=0, tiled=True)
        back = lax.rem(ep_index - sign * steps_ahead + ep, ep)
        return moved[back].reshape(rows.shape)

    def gathered(value):
        if square:
            return pieces_over(value, "tp")
        return [lax.all_gather(value, "tp", axis=1, tiled=True)]

    def times(pieces, w):
        return dot_pieces(pieces, w, tp_index) if square else dot(pieces[0], w)

    arrived = []
    for c in range(chunks):
        slots = c * part + jnp.arange(part, dtype=jnp.int32)
        pick = (rank_rows[:, None, :] == slots[None, :, None]).astype(bf16)
        packed = dot(pick.reshape(ep * part, tokens), own).astype(bf16)
        arrived.append(gathered(exchange(packed, 1)))
    hidden = []
    for c in range(chunks):
        gate_proj, up_proj = times(arrived[c], gate_w), times(arrived[c], up_w)
        hidden.append(gathered((jax.nn.silu(gate_proj) * up_proj).astype(bf16)))
    total = None
    for c in range(chunks):
        results = times(hidden[c], down_w).astype(bf16)
        returned = exchange(results, -1)
        slots = c * part + jnp.arange(part, dtype=jnp.int32)
        at = rank[:, :, None] == slots[None, None, :]
        for w in (weight_top, weight_low):
            mix = jnp.where(at, w[:, :, None], 0.0).astype(bf16).reshape(tokens, ep * part)
            term = dot(mix, returned)
            total = term if total is None else total + term
    return total.astype(bf16)


def local(*args):
    moe_out = experts(*args[9:])
    mixer_out = mixer(*args[:9])
    return (mixer_out, moe_out)


def solution(mesh):
    placed = (
        P("ep", None),
        P(),
        P(None, "tp"),
        P(None, "tp"),
        P(None, "tp"),
        P("tp", None, None),
        P("tp", None, None),
        P("tp"),
        P("ep", "tp"),
        P("ep", None),
        P(),
        P("ep", None),
        P("ep", None),
        P("ep", None, "tp"),
        P("ep", None, "tp"),
        P("ep", None, "tp"),
    )
    return jax.shard_map(
        local, mesh=mesh, in_specs=placed, out_specs=(P("ep", "tp"), P("ep", "tp")), check_vma=False
    )
```

```python
import jax
import jax.numpy as jnp
from jax import lax
from jax.experimental import pallas as pl
from jax.experimental.pallas import tpu as pltpu
from jax.sharding import PartitionSpec as P

epsilon = 1e-06
lru_scale = 8.0
chunks = 2
bf16, f32 = jnp.bfloat16, jnp.float32


def norm_rows(rows, gain):
    widened = rows.astype(f32)
    scaled = widened * lax.rsqrt(jnp.mean(widened * widened, axis=-1, keepdims=True) + epsilon)
    return (scaled * gain[None, :]).astype(bf16)


def from_behind(value, axis, by):
    count = lax.axis_size(axis)
    pairs = [(i, i + by) for i in range(count) if i + by < count]
    return lax.ppermute(value, axis, pairs)


def swap(value, axis, bit):
    count = lax.axis_size(axis)
    return lax.ppermute(value, axis, [(i, i ^ bit) for i in range(count)])


def pieces_over(value, axis, first):
    near = {bit: swap(value, axis, bit) for bit in (first, 3 - first)}
    return [value, near[1], near[2], swap(near[first], axis, 3 - first)]


def dot(a, b):
    return jnp.dot(a, b, preferred_element_type=f32)


def dot_pieces(pieces, weight, index):
    depth = pieces[0].shape[1]
    total = None
    for m, piece in enumerate(pieces):
        part = dot(piece, lax.dynamic_slice_in_dim(weight, (index ^ m) * depth, depth, 0))
        total = part if total is None else total + part
    return total


def scan_kernel(a_ref, b_ref, through_ref, state_ref):
    rows, lanes = a_ref.shape
    a, b = a_ref[...], b_ref[...]
    row = lax.broadcasted_iota(jnp.int32, (rows, lanes), 0)
    step = 1
    while step < rows:
        if step % 8 == 0:
            a_back = jnp.concatenate([jnp.ones((step, lanes), f32), a[: rows - step]], axis=0)
            b_back = jnp.concatenate([jnp.zeros((step, lanes), f32), b[: rows - step]], axis=0)
        else:
            a_back = jnp.where(row >= step, pltpu.roll(a, step, 0), 1.0)
            b_back = jnp.where(row >= step, pltpu.roll(b, step, 0), 0.0)
        b = a * b_back + b
        a = a * a_back
        step *= 2
    through_ref[...] = a
    state_ref[...] = b


def local_scan(a, b):
    rows, width = a.shape
    spec = pl.BlockSpec((rows, 128), lambda i: (0, i))
    shape = jax.ShapeDtypeStruct((rows, width), f32)
    return pl.pallas_call(
        scan_kernel,
        grid=(width // 128,),
        in_specs=[spec, spec],
        out_specs=[spec, spec],
        out_shape=[shape, shape],
        cost_estimate=pl.CostEstimate(
            flops=rows * width * 32, bytes_accessed=rows * width * 16, transcendentals=0
        ),
        name="local_scan",
    )(a, b)


def carried_in(through, state):
    index, count = lax.axis_index("ep"), lax.axis_size("ep")
    pair = jnp.stack([through, state])
    step = 1
    while step < count:
        back = from_behind(pair, "ep", step)
        a, b = pair[0], pair[1]
        joined = jnp.stack([a * back[0], a * back[1] + b])
        pair = jnp.where(index >= step, joined, pair)
        step *= 2
    return from_behind(pair[1:2], "ep", 1)[0]


def mixer(
    mix_in, mix_gain, w_in_x, w_in_y, conv_taps, recur_gate_w, input_gate_w, decay_logit, decay_shift
):
    row_count = mix_in.shape[0]
    width_dev = w_in_x.shape[1]
    heads_dev, block_size = recur_gate_w.shape[:2]
    tap_count = conv_taps.shape[0]
    mixer_rows = norm_rows(mix_in, mix_gain)
    x_branch = dot(mixer_rows, w_in_x).astype(bf16)
    y_branch = dot(mixer_rows, w_in_y).astype(bf16)
    previous = from_behind(x_branch[row_count - (tap_count - 1) :], "ep", 1)
    padded = jnp.concatenate([previous, x_branch], axis=0)
    conv_sum = jnp.zeros((row_count, width_dev), f32)
    for tap_index in range(tap_count):
        conv_sum = conv_sum + conv_taps[tap_index][None, :] * padded[
            tap_index : tap_index + row_count
        ].astype(f32)
    x_conv = conv_sum.astype(bf16)
    gates = []
    for weight in (recur_gate_w, input_gate_w):
        blocks = [
            dot(x_conv[:, h * block_size : (h + 1) * block_size], weight[h])
            for h in range(heads_dev)
        ]
        gates.append(jnp.concatenate(blocks, axis=1))
    gate_a, gate_x = gates
    log_decay = (
        -lru_scale * jax.nn.sigmoid(gate_a) * jax.nn.softplus(-decay_logit)[None, :] + decay_shift
    )
    drive = jnp.sqrt(-jnp.expm1(2.0 * log_decay)) * jax.nn.sigmoid(gate_x) * x_conv.astype(f32)
    through, local_state = local_scan(jnp.exp(log_decay), drive)
    carried = carried_in(through[row_count - 1], local_state[row_count - 1])
    lru_state = local_state + through * carried[None, :]
    return (lru_state * jax.nn.gelu(y_branch.astype(f32))).astype(bf16)


def experts(moe_in, moe_gain, routes, route_weight, expert_gate, expert_up, expert_down):
    ep, tp = lax.axis_size("ep"), lax.axis_size("tp")
    tp_index = lax.axis_index("tp")
    moe_rows = norm_rows(moe_in, moe_gain)
    tokens, features = moe_rows.shape
    capacity = 2 * tokens * routes.shape[1] // ep
    width = features // tp
    own = lax.dynamic_slice_in_dim(moe_rows, tp_index * width, width, 1)

    chosen = routes[:, :, None] == jnp.arange(ep, dtype=jnp.int32)[None, None, :]
    named = jnp.any(chosen, axis=1)
    order = jnp.arange(tokens, dtype=jnp.int32)
    before = (order[None, :] < order[:, None]).astype(bf16)
    rank = dot(before, named.astype(bf16)).astype(jnp.int32)
    rank = jnp.where(named, rank, -1)
    share = route_weight / jnp.sum(route_weight, axis=1, keepdims=True)
    weight = jnp.sum(jnp.where(chosen, share[:, :, None], 0.0), axis=1)
    weight_top = lax.reduce_precision(weight, 8, 7)
    weight_low = weight - weight_top
    rank_rows = rank.T

    part = capacity // chunks
    gate_w, up_w, down_w = expert_gate[0], expert_up[0], expert_down[0]
    square = tp == 4

    def exchange(rows):
        blocks = rows.reshape(ep, part, rows.shape[1])
        moved = lax.all_to_all(blocks, "ep", split_axis=0, concat_axis=0, tiled=True)
        return moved.reshape(rows.shape)

    def gathered(value, c):
        if square:
            return pieces_over(value, "tp", 1 + c % 2)
        return [lax.all_gather(value, "tp", axis=1, tiled=True)]

    def times(pieces, w):
        return dot_pieces(pieces, w, tp_index) if square else dot(pieces[0], w)

    arrived = []
    for c in range(chunks):
        slots = c * part + jnp.arange(part, dtype=jnp.int32)
        pick = (rank_rows[:, None, :] == slots[None, :, None]).astype(bf16)
        packed = dot(pick.reshape(ep * part, tokens), own).astype(bf16)
        arrived.append(gathered(exchange(packed), c))
    hidden = []
    for c in range(chunks):
        gate_proj, up_proj = times(arrived[c], gate_w), times(arrived[c], up_w)
        hidden.append(gathered((jax.nn.silu(gate_proj) * up_proj).astype(bf16), c))
    total = None
    for c in range(chunks):
        results = times(hidden[c], down_w).astype(bf16)
        returned = exchange(results)
        slots = c * part + jnp.arange(part, dtype=jnp.int32)
        at = rank[:, :, None] == slots[None, None, :]
        for w in (weight_top, weight_low):
            mix = jnp.where(at, w[:, :, None], 0.0).astype(bf16).reshape(tokens, ep * part)
            term = dot(mix, returned)
            total = term if total is None else total + term
    return total.astype(bf16)


def local(*args):
    moe_out = experts(*args[9:])
    mixer_out = mixer(*args[:9])
    return (mixer_out, moe_out)


def solution(mesh):
    placed = (
        P("ep", None),
        P(),
        P(None, "tp"),
        P(None, "tp"),
        P(None, "tp"),
        P("tp", None, None),
        P("tp", None, None),
        P("tp"),
        P("ep", "tp"),
        P("ep", None),
        P(),
        P("ep", None),
        P("ep", None),
        P("ep", None, "tp"),
        P("ep", None, "tp"),
        P("ep", None, "tp"),
    )
    return jax.shard_map(
        local, mesh=mesh, in_specs=placed, out_specs=(P("ep", "tp"), P("ep", "tp")), check_vma=False
    )
```

```python
import jax
import jax.numpy as jnp
from jax import lax
from jax.experimental import pallas as pl
from jax.experimental.pallas import tpu as pltpu
from jax.sharding import PartitionSpec as P

epsilon = 1e-06
lru_scale = 8.0
chunks = 2
bf16, f32 = jnp.bfloat16, jnp.float32


def norm_rows(rows, gain):
    widened = rows.astype(f32)
    scaled = widened * lax.rsqrt(jnp.mean(widened * widened, axis=-1, keepdims=True) + epsilon)
    return (scaled * gain[None, :]).astype(bf16)


def from_behind(value, axis, by):
    count = lax.axis_size(axis)
    pairs = [(i, i + by) for i in range(count) if i + by < count]
    return lax.ppermute(value, axis, pairs)


def swap(value, axis, bit):
    count = lax.axis_size(axis)
    return lax.ppermute(value, axis, [(i, i ^ bit) for i in range(count)])


def pieces_over(value, axis):
    return [value] + [swap(value, axis, m) for m in (1, 2, 3)]


def dot(a, b):
    return jnp.dot(a, b, preferred_element_type=f32)


def dot_pieces(pieces, weight, index):
    depth = pieces[0].shape[1]
    total = None
    for m, piece in enumerate(pieces):
        part = dot(piece, lax.dynamic_slice_in_dim(weight, (index ^ m) * depth, depth, 0))
        total = part if total is None else total + part
    return total


def scan_kernel(a_ref, b_ref, through_ref, state_ref):
    rows, lanes = a_ref.shape
    a, b = a_ref[...], b_ref[...]
    row = lax.broadcasted_iota(jnp.int32, (rows, lanes), 0)
    step = 1
    while step < rows:
        if step % 8 == 0:
            a_back = jnp.concatenate([jnp.ones((step, lanes), f32), a[: rows - step]], axis=0)
            b_back = jnp.concatenate([jnp.zeros((step, lanes), f32), b[: rows - step]], axis=0)
        else:
            a_back = jnp.where(row >= step, pltpu.roll(a, step, 0), 1.0)
            b_back = jnp.where(row >= step, pltpu.roll(b, step, 0), 0.0)
        b = a * b_back + b
        a = a * a_back
        step *= 2
    through_ref[...] = a
    state_ref[...] = b


def local_scan(a, b):
    rows, width = a.shape
    spec = pl.BlockSpec((rows, 128), lambda i: (0, i))
    shape = jax.ShapeDtypeStruct((rows, width), f32)
    return pl.pallas_call(
        scan_kernel,
        grid=(width // 128,),
        in_specs=[spec, spec],
        out_specs=[spec, spec],
        out_shape=[shape, shape],
        cost_estimate=pl.CostEstimate(
            flops=rows * width * 32, bytes_accessed=rows * width * 16, transcendentals=0
        ),
        name="local_scan",
    )(a, b)


def carried_in(pair):
    index, count = lax.axis_index("ep"), lax.axis_size("ep")
    step = 1
    while step < count:
        back = from_behind(pair, "ep", step)
        a, b = pair[0], pair[1]
        joined = jnp.stack([a * back[0], a * back[1] + b])
        pair = jnp.where(index >= step, joined, pair)
        step *= 2
    return from_behind(pair[1:2], "ep", 1)[0]


def mixer(
    mix_in, mix_gain, w_in_x, w_in_y, conv_taps, recur_gate_w, input_gate_w, decay_logit, decay_shift
):
    row_count = mix_in.shape[0]
    width_dev = w_in_x.shape[1]
    heads_dev, block_size = recur_gate_w.shape[:2]
    tap_count = conv_taps.shape[0]
    mixer_rows = norm_rows(mix_in, mix_gain)
    x_branch = dot(mixer_rows, w_in_x).astype(bf16)
    y_branch = dot(mixer_rows, w_in_y).astype(bf16)
    previous = from_behind(x_branch[row_count - (tap_count - 1) :], "ep", 1)
    padded = jnp.concatenate([previous, x_branch], axis=0)
    conv_sum = jnp.zeros((row_count, width_dev), f32)
    for tap_index in range(tap_count):
        conv_sum = conv_sum + conv_taps[tap_index][None, :] * padded[
            tap_index : tap_index + row_count
        ].astype(f32)
    x_conv = conv_sum.astype(bf16)
    gates = []
    for weight in (recur_gate_w, input_gate_w):
        blocks = [
            dot(x_conv[:, h * block_size : (h + 1) * block_size], weight[h])
            for h in range(heads_dev)
        ]
        gates.append(jnp.concatenate(blocks, axis=1))
    gate_a, gate_x = gates
    log_decay = (
        -lru_scale * jax.nn.sigmoid(gate_a) * jax.nn.softplus(-decay_logit)[None, :] + decay_shift
    )
    drive = jnp.sqrt(-jnp.expm1(2.0 * log_decay)) * jax.nn.sigmoid(gate_x) * x_conv.astype(f32)
    through, local_state = local_scan(jnp.exp(log_decay), drive)
    return through, local_state, y_branch


def mixer_end(through, local_state, y_branch, pair):
    lru_state = local_state + through * carried_in(pair)[None, :]
    return (lru_state * jax.nn.gelu(y_branch.astype(f32))).astype(bf16)


def experts(pair, moe_in, moe_gain, routes, route_weight, expert_gate, expert_up, expert_down):
    ep, tp = lax.axis_size("ep"), lax.axis_size("tp")
    tp_index = lax.axis_index("tp")
    moe_rows = norm_rows(moe_in, moe_gain)
    tokens, features = moe_rows.shape
    capacity = 2 * tokens * routes.shape[1] // ep
    width = features // tp
    own = lax.dynamic_slice_in_dim(moe_rows, tp_index * width, width, 1)

    chosen = routes[:, :, None] == jnp.arange(ep, dtype=jnp.int32)[None, None, :]
    named = jnp.any(chosen, axis=1)
    order = jnp.arange(tokens, dtype=jnp.int32)
    before = (order[None, :] < order[:, None]).astype(bf16)
    rank = dot(before, named.astype(bf16)).astype(jnp.int32)
    rank = jnp.where(named, rank, -1)
    share = route_weight / jnp.sum(route_weight, axis=1, keepdims=True)
    weight = jnp.sum(jnp.where(chosen, share[:, :, None], 0.0), axis=1)
    weight_top = lax.reduce_precision(weight, 8, 7)
    weight_low = weight - weight_top
    rank_rows = rank.T

    part = capacity // chunks
    gate_w, up_w, down_w = expert_gate[0], expert_up[0], expert_down[0]
    square = tp == 4

    def exchange(rows):
        blocks = rows.reshape(ep, part, rows.shape[1])
        moved = lax.all_to_all(blocks, "ep", split_axis=0, concat_axis=0, tiled=True)
        return moved.reshape(rows.shape)

    def gathered(value):
        if square:
            return pieces_over(value, "tp")
        return [lax.all_gather(value, "tp", axis=1, tiled=True)]

    def times(pieces, w):
        return dot_pieces(pieces, w, tp_index) if square else dot(pieces[0], w)

    arrived = []
    for c in range(chunks):
        slots = c * part + jnp.arange(part, dtype=jnp.int32)
        pick = (rank_rows[:, None, :] == slots[None, :, None]).astype(bf16)
        packed = dot(pick.reshape(ep * part, tokens), own).astype(bf16)
        arrived.append(gathered(exchange(packed)))
    hidden = []
    for c in range(chunks):
        gate_proj, up_proj = times(arrived[c], gate_w), times(arrived[c], up_w)
        hidden.append(gathered((jax.nn.silu(gate_proj) * up_proj).astype(bf16)))
    hidden[0][-3 % len(hidden[0])], pair = lax.optimization_barrier(
        (hidden[0][-3 % len(hidden[0])], pair)
    )
    total = None
    for c in range(chunks):
        results = times(hidden[c], down_w).astype(bf16)
        returned = exchange(results)
        slots = c * part + jnp.arange(part, dtype=jnp.int32)
        at = rank[:, :, None] == slots[None, None, :]
        for w in (weight_top, weight_low):
            mix = jnp.where(at, w[:, :, None], 0.0).astype(bf16).reshape(tokens, ep * part)
            term = dot(mix, returned)
            total = term if total is None else total + term
    return total.astype(bf16), pair


def local(*args):
    through, local_state, y_branch = mixer(*args[:9])
    pair = jnp.stack([through[-1], local_state[-1]])
    moe_out, pair = experts(pair, *args[9:])
    return (mixer_end(through, local_state, y_branch, pair), moe_out)


def solution(mesh):
    placed = (
        P("ep", None),
        P(),
        P(None, "tp"),
        P(None, "tp"),
        P(None, "tp"),
        P("tp", None, None),
        P("tp", None, None),
        P("tp"),
        P("ep", "tp"),
        P("ep", None),
        P(),
        P("ep", None),
        P("ep", None),
        P("ep", None, "tp"),
        P("ep", None, "tp"),
        P("ep", None, "tp"),
    )
    return jax.shard_map(
        local, mesh=mesh, in_specs=placed, out_specs=(P("ep", "tp"), P("ep", "tp")), check_vma=False
    )
```
